256 devices in a mesh: dp: 4 (over y), kv: 32 (over z, x), tp: 2 (over core).
Axes of the slice: x: 4, y: 4, z: 8, core: 2. Of those that a mesh axis runs over, the one named last changes fastest.
Arguments:
- tokens: bfloat16 [4, 24576, 2048], P('dp', 'kv'), may hold values from -60 to 60
- query_weight: bfloat16 [2048, 1024], P(None, 'tp'), may hold values from -0.125 to 0.125
- key_weight: bfloat16 [2048, 256], P(None, 'tp'), may hold values from -0.125 to 0.125
- value_weight: bfloat16 [2048, 256], P(None, 'tp'), may hold values from -0.125 to 0.125
- out_weight: bfloat16 [1024, 2048], P('tp'), may hold values from -3 to 3
- norm_gain: float32 [2048], P('tp'), may hold values from 0.1 to 1.9
- chosen_owner: int32 [4, 192, 16], P('dp'), may hold values from -1 to 31, as said below
- chosen_part: int32 [4, 192, 16], P('dp'), may hold values from 0 to 11, as said below
Outputs:
- attended: bfloat16 [4, 24576, 2048], P('dp', 'kv', 'tp')
The draws below stay inside these ranges and needn't reach their ends.
Inputs may be any that keep to these rules, and one draw needn't show every extreme that they name: `chosen_owner`: within a row the indices other than -1 are different. Every named key block lies wholly before its query block's first position. Among the 6 rows of one index of kv, no index is named by more than 6 rows. `chosen_part`: 0 where the owner is -1.
All inputs are finite; a program needn't handle non-finite values.
Results may differ from the reference program's by a relative error of at most 0.014.
The reference program's roundings to bfloat16 on the way count: a program that leaves them out, or rounds other values in their place, can miss the bound.
Values may be sent and summed in bfloat16 or wider, within the bound.
A program may use at most 128 MiB of HBM per device.

```python
import jax
import jax.numpy as jnp
from jax import lax

D = 2048
HEADS = 16
KV_HEADS = 4
HEAD_DIM = 64
QUERY_BLOCK = 128
KEY_BLOCK = 64
SEQS = 4
SEQ = 24576
QBLOCKS = 192
QBLOCKS_DEV = 6
KBLOCKS_DEV = 12
CHOSEN = 16
N_KV = 32
N_TP = 2


def draw_tokens(key, part):
    base = jax.random.normal(jax.random.fold_in(key, 11), (SEQS, SEQ, D), jnp.float32)
    base = jnp.clip(base, -6.0, 6.0)
    return base.astype(jnp.bfloat16)


def draw_out_weight(key, part):
    base = jax.random.normal(jax.random.fold_in(key, 21), (HEADS * HEAD_DIM, D), jnp.float32)
    base = jnp.clip(base, -6.0, 6.0) * (HEADS * HEAD_DIM) ** (-0.5)
    column = jnp.arange(D, dtype=jnp.float32) / D
    jitter = jnp.exp(jax.random.uniform(jax.random.fold_in(key, 22), (D,), jnp.float32, -0.5, 0.5))
    rising = 3.0 ** column
    return (base * (rising * jitter)[None, :] * 0.5).astype(jnp.bfloat16)


def chosen_pair(key):
    block_ids = jnp.arange(QBLOCKS, dtype=jnp.int32)
    device_ids = block_ids // QBLOCKS_DEV
    local_ids = block_ids % QBLOCKS_DEV
    owners = jnp.arange(N_KV, dtype=jnp.int32)
    earlier = owners[None, :] < device_ids[:, None]
    itself = jnp.logical_and(owners[None, :] == device_ids[:, None], local_ids[:, None] > 0)
    allowed = jnp.logical_or(earlier, itself)
    forced = jnp.logical_or(jnp.logical_or(owners[None, :] == 0, owners[None, :] == device_ids[:, None] - 1), jnp.logical_or(owners[None, :] == device_ids[:, None] - N_KV // 2, owners[None, :] == device_ids[:, None]))
    forced = jnp.logical_and(forced, allowed)
    noise = jax.random.randint(jax.random.fold_in(key, 31), (SEQS, QBLOCKS, N_KV), 0, 16384)
    scores = noise + (N_KV - owners)[None, None, :] * (16384 // N_KV) + forced[None].astype(jnp.int32) * 1048576
    scores = jnp.where(allowed[None], scores, -2097152)
    scores = scores * 64 + owners[None, None, :]
    picked = lax.top_k(scores, CHOSEN)[1].astype(jnp.int32)
    valid = jnp.take_along_axis(jnp.broadcast_to(allowed[None], (SEQS, QBLOCKS, N_KV)), picked, axis=2)
    owner_out = jnp.where(valid, picked, -1).astype(jnp.int32)
    limit = jnp.where(picked == device_ids[None, :, None], QUERY_BLOCK // KEY_BLOCK * local_ids[None, :, None], KBLOCKS_DEV)
    limit = jnp.maximum(limit, 1)
    raw_part = jax.random.randint(jax.random.fold_in(key, 32), (SEQS, QBLOCKS, CHOSEN), 0, 1048576)
    part_out = jnp.where(valid, raw_part % limit, 0).astype(jnp.int32)
    return (owner_out, part_out)


def draw_chosen_owner(key, part):
    return chosen_pair(jax.random.fold_in(key, 41))[0]


def draw_chosen_part(key, part):
    return chosen_pair(jax.random.fold_in(key, 41))[1]


def level_of(own_key, dims, cuts, least, high):
    gain, own = 1.0, jax.random.fold_in(own_key, 6)
    for axis_at, parts in cuts:
        draws = jnp.exp(jax.random.uniform(jax.random.fold_in(own, axis_at), (parts,), jnp.float32, least / len(cuts), high / len(cuts)))
        gain = gain * jnp.repeat(draws, dims[axis_at] // parts).reshape([-1 if axis == axis_at else 1 for axis in range(len(dims))])
    return gain


def bell_draw(rng, shape, deviation, bound, split=(), held_as=jnp.bfloat16):
    factor_of = level_of(rng, shape, split, -0.22, 0.18) if split else 1.0
    drawn = jax.random.normal(rng, shape, jnp.float32) * deviation * factor_of
    return jnp.minimum(jnp.maximum(drawn, -bound), bound).astype(held_as)


def setup_inputs(seed: int = 0) -> dict:
    keys = jax.random.split(jax.random.key(seed), 9)
    tokens = draw_tokens(jax.random.fold_in(keys[8], 71), 0)
    query_weight = bell_draw(keys[1], (D, HEADS * HEAD_DIM), D ** -0.5, 0.125, ((1, 2),))
    key_weight = bell_draw(keys[2], (D, KV_HEADS * HEAD_DIM), D ** -0.5, 0.125, ((1, 2),))
    value_weight = bell_draw(keys[3], (D, KV_HEADS * HEAD_DIM), D ** -0.5, 0.125, ((1, 2),))
    out_weight = draw_out_weight(jax.random.fold_in(keys[8], 71), 0)
    norm_gain = jnp.clip(1.0 + 0.18 * jax.random.normal(keys[5], (D,), jnp.float32), 0.1, 1.9)
    chosen_owner = draw_chosen_owner(jax.random.fold_in(keys[8], 71), 0)
    chosen_part = draw_chosen_part(jax.random.fold_in(keys[8], 71), 0)
    return {"tokens": tokens, "query_weight": query_weight, "key_weight": key_weight, "value_weight": value_weight, "out_weight": out_weight, "norm_gain": norm_gain, "chosen_owner": chosen_owner, "chosen_part": chosen_part}


rope_base = 10000.0
norm_eps = 1e-06

def rotate(head_rows, positions):
    half_dim = head_rows.shape[-1] // 2
    frequency = rope_base ** (-jnp.arange(half_dim, dtype=jnp.float32) / half_dim)
    angles = positions.astype(jnp.float32)[:, None] * frequency
    cosine = jnp.cos(angles)[:, None, :]
    sine_part = jnp.sin(angles)[:, None, :]
    first_half = head_rows[..., :half_dim]
    second_half = head_rows[..., half_dim:]
    return jnp.concatenate([first_half * cosine - second_half * sine_part, second_half * cosine + first_half * sine_part], axis=-1)

def reference(tokens, query_weight, key_weight, value_weight, out_weight, norm_gain, chosen_owner, chosen_part):
    group_size = HEADS // KV_HEADS
    lower_mask = jnp.arange(QUERY_BLOCK)[:, None] >= jnp.arange(QUERY_BLOCK)[None, :]

    def one_sequence(seq_items):
        row_data, owner_ids, part_ids = seq_items
        positions = jnp.arange(SEQ, dtype=jnp.int32)
        queries = rotate(jnp.dot(row_data, query_weight, preferred_element_type=jnp.float32).reshape(SEQ, HEADS, HEAD_DIM), positions).astype(jnp.bfloat16)
        key_rows = rotate(jnp.dot(row_data, key_weight, preferred_element_type=jnp.float32).reshape(SEQ, KV_HEADS, HEAD_DIM), positions).astype(jnp.bfloat16)
        value_rows = jnp.dot(row_data, value_weight, preferred_element_type=jnp.float32).astype(jnp.bfloat16).reshape(SEQ, KV_HEADS, HEAD_DIM)
        key_blocks = key_rows.reshape(SEQ // KEY_BLOCK, KEY_BLOCK, KV_HEADS, HEAD_DIM)
        value_blocks = value_rows.reshape(SEQ // KEY_BLOCK, KEY_BLOCK, KV_HEADS, HEAD_DIM)
        slot_valid = owner_ids >= 0
        chosen_ids = jnp.where(slot_valid, owner_ids * KBLOCKS_DEV + part_ids, 0).astype(jnp.int32)

        def one_block(block_index):
            block_start = (block_index * QUERY_BLOCK).astype(jnp.int32)
            picked_ids = chosen_ids[block_index]
            valid_row = slot_valid[block_index]
            block_queries = lax.dynamic_slice_in_dim(queries, block_start, QUERY_BLOCK, 0).reshape(QUERY_BLOCK, KV_HEADS, group_size, HEAD_DIM).astype(jnp.float32)
            own_keys = lax.dynamic_slice_in_dim(key_rows, block_start, QUERY_BLOCK, 0)
            own_values = lax.dynamic_slice_in_dim(value_rows, block_start, QUERY_BLOCK, 0)
            chosen_keys = key_blocks[picked_ids].reshape(CHOSEN * KEY_BLOCK, KV_HEADS, HEAD_DIM)
            chosen_values = value_blocks[picked_ids].reshape(CHOSEN * KEY_BLOCK, KV_HEADS, HEAD_DIM)
            all_keys = jnp.concatenate([chosen_keys, own_keys], axis=0).astype(jnp.float32)
            all_values = jnp.concatenate([chosen_values, own_values], axis=0).astype(jnp.float32)
            key_valid = jnp.broadcast_to(valid_row[:, None], (CHOSEN, KEY_BLOCK)).reshape(CHOSEN * KEY_BLOCK)
            far_mask = jnp.broadcast_to(key_valid[None, :], (QUERY_BLOCK, CHOSEN * KEY_BLOCK))
            full_mask = jnp.concatenate([far_mask, lower_mask], axis=1)
            scores = jnp.einsum('qngd,knd->ngqk', block_queries, all_keys) * HEAD_DIM ** (-0.5)
            scores = jnp.where(full_mask[None, None], scores, -jnp.inf)
            row_max = lax.optimization_barrier(jnp.max(scores, axis=-1, keepdims=True))
            weights = jnp.exp(scores - row_max)
            weights = (weights / lax.optimization_barrier(jnp.sum(weights, axis=-1, keepdims=True))).astype(jnp.bfloat16)
            mixed_out = jnp.einsum('ngqk,knd->qngd', weights.astype(jnp.float32), all_values)
            return mixed_out.reshape(QUERY_BLOCK, HEADS * HEAD_DIM).astype(jnp.bfloat16)
        mixed_rows = lax.map(one_block, jnp.arange(QBLOCKS, dtype=jnp.int32)).reshape(SEQ, HEADS * HEAD_DIM)
        share_cols = HEADS * HEAD_DIM // N_TP
        summed = jnp.zeros((SEQ, D), jnp.float32)
        for member in range(N_TP):
            partial_value = jnp.dot(mixed_rows[:, member * share_cols:(member + 1) * share_cols], out_weight[member * share_cols:(member + 1) * share_cols], preferred_element_type=jnp.float32).astype(jnp.bfloat16)
            summed = summed + lax.optimization_barrier(partial_value).astype(jnp.float32)
        mean_sq = lax.optimization_barrier(jnp.mean(summed * summed, axis=1, keepdims=True))
        return (summed * lax.rsqrt(mean_sq + norm_eps) * norm_gain.astype(jnp.float32)).astype(jnp.bfloat16)
    return lax.map(one_sequence, (tokens, chosen_owner, chosen_part))
```

```python
import jax
import jax.numpy as jnp
from jax import lax
from jax.experimental import pallas as pl
from jax.experimental.pallas import tpu as pltpu
from jax.sharding import PartitionSpec as P

D = 2048
HEAD_DIM = 64
QUERY_BLOCK = 128
KEY_BLOCK = 64
NZ = 8
NX = 4
ROWS = 6
PARTS = 12
CHOSEN = 16
FULL = NZ * PARTS
SEL = NZ * ROWS
BLOCKS = 2 * FULL + 2 * SEL
rope_base = 10000.0
norm_eps = 1e-06
MESH = pl.DeviceIdType.MESH
LOG2E = 1.4426950408889634


def split_up(x, dim, count):
    before, after = (x.shape[:dim], x.shape[dim + 1 :])
    return jnp.moveaxis(x.reshape(*before, count, -1, *after), dim, 0)


def summed_on_arrival(x, axis, dim):
    count = lax.axis_size(axis)
    blocks = lax.all_to_all(split_up(x, dim, count), axis, 0, 0, tiled=True)
    return jnp.sum(blocks.astype(jnp.float32), axis=0)


def turned(u, cosine, sine, low_half):
    other = jnp.where(low_half, pltpu.roll(u, 96, 1), pltpu.roll(u, 32, 1))
    return u * cosine + other * sine


def project_kernel(x_ref, wq_ref, wk_ref, wv_ref, cos_ref, sin_ref, q_ref, k_ref, v_ref):
    x = x_ref[...]
    cosine, sine = cos_ref[...], sin_ref[...]
    lane = lax.broadcasted_iota(jnp.int32, cosine.shape, 1)
    low_half = (lane % HEAD_DIM) < HEAD_DIM // 2
    first_head = lane < HEAD_DIM
    keys = jnp.dot(x, wk_ref[...], preferred_element_type=jnp.float32)
    k_ref[...] = turned(keys, cosine, sine, low_half).astype(jnp.bfloat16)
    v_ref[...] = jnp.dot(x, wv_ref[...], preferred_element_type=jnp.float32).astype(jnp.bfloat16)
    q = jnp.dot(x, wq_ref[...], preferred_element_type=jnp.float32)
    raw = [turned(q[:, 128 * i : 128 * (i + 1)], cosine, sine, low_half) for i in range(4)]
    swapped = [pltpu.roll(u, 64, 1) for u in raw]
    paired = [
        jnp.where(first_head, raw[0], swapped[2]),
        jnp.where(first_head, swapped[0], raw[2]),
        jnp.where(first_head, raw[1], swapped[3]),
        jnp.where(first_head, swapped[1], raw[3]),
    ]
    for i in range(4):
        q_ref[:, 128 * i : 128 * (i + 1)] = paired[i].astype(jnp.bfloat16)


def exchange_kernel(t_ref, k_ref, v_ref, kb_ref, vb_ref, whole, stage, zsend, zrecv, nsend, nrecv, ssend, srecv):
    me = lax.axis_index("kv")
    z, x = me // NX, me % NX
    up = ((z + 1) % NZ) * NX + x
    down = ((z + NZ - 1) % NZ) * NX + x
    right = z * NX + (x + 1) % NX
    left = z * NX + (x + NX - 1) % NX
    xr, xl = (x + 1) % NX, (x + NX - 1) % NX
    barrier = pltpu.get_barrier_semaphore()
    for peer in (up, down, right, left):
        pl.semaphore_signal(barrier, inc=1, device_id={"kv": peer}, device_id_type=MESH)
    pl.semaphore_wait(barrier, 4)
    sent = []

    def send(src, dst, ssem, rsem, peer):
        copy = pltpu.make_async_remote_copy(
            src_ref=src, dst_ref=dst, send_sem=ssem, recv_sem=rsem,
            device_id={"kv": peer}, device_id_type=MESH,
        )
        copy.start()
        sent.append(copy)
        return copy

    bufs = (kb_ref, vb_ref, kb_ref, vb_ref)
    bases = (0, 0, FULL, FULL)

    def chunk(kind, slot):
        return bufs[kind].at[pl.ds(bases[kind] + slot * PARTS, PARTS)]

    arrivals = {}

    def forward(kind, direction, step, src):
        slot = step if direction == 0 else NZ - step
        arrivals[direction, step, kind] = send(
            src, chunk(kind, slot), zsend.at[direction, step - 1, kind],
            zrecv.at[direction, step - 1, kind], up if direction == 0 else down,
        )

    def pick(kind, slot):
        buf = bufs[kind]
        owner_x = (x, x, xl, xr)[kind]
        dest_x, dest = ((xl, left), (xr, right), (xr, right), (xl, left))[kind]
        owner = ((z + NZ - slot) % NZ) * NX + owner_x
        base = bases[kind] + slot * PARTS
        whole[...] = buf[base : base + PARTS]
        for r in range(ROWS):
            part = t_ref[(dest_x * ROWS + r) * (NZ * NX) + owner]
            stage[slot, kind, r] = whole[part]
        place = 2 * FULL + (SEL if kind >= 2 else 0) + slot * ROWS
        return send(
            stage.at[slot, kind], buf.at[pl.ds(place, ROWS)],
            ssend.at[slot, kind], srecv.at[slot, kind], dest,
        )

    for direction in range(2):
        forward(0, direction, 1, k_ref)
        forward(1, direction, 1, v_ref)
    near = [
        send(k_ref, chunk(2, 0), nsend.at[0], nrecv.at[0], right),
        send(v_ref, chunk(3, 0), nsend.at[1], nrecv.at[1], left),
    ]
    kb_ref[0:PARTS] = k_ref[...]
    vb_ref[0:PARTS] = v_ref[...]
    picked = [pick(0, 0), pick(1, 0)]
    for kind in (2, 3):
        near[kind - 2].wait_recv()
        forward(kind, 0, 1, chunk(kind, 0))
        forward(kind, 1, 1, chunk(kind, 0))
        picked.append(pick(kind, 0))
    half = NZ // 2
    for step in range(1, half + 1):
        for kind in range(4):
            ready = []
            for direction in range(2):
                if (direction, step, kind) not in arrivals:
                    continue
                arrivals[direction, step, kind].wait_recv()
                slot = step if direction == 0 else NZ - step
                ready.append(slot)
                if step + 1 < half or (step + 1 == half and kind % 2 == direction):
                    forward(kind, direction, step + 1, chunk(kind, slot))
            for slot in ready:
                picked.append(pick(kind, slot))
    for copy in picked:
        copy.wait_recv()
    for copy in sent:
        copy.wait_send()


def attend_kernel(kidx_ref, vidx_ref, bias_ref, q_ref, k_ref, v_ref, kb_ref, vb_ref, out_ref, keys, values, ksem, vsem):
    b = pl.program_id(0)
    count = pl.num_programs(0)

    def fetch(row, slot, start):
        for s in range(CHOSEN):
            kcopy = pltpu.make_async_copy(
                kb_ref.at[kidx_ref[row * CHOSEN + s]],
                keys.at[slot, pl.ds(s * KEY_BLOCK, KEY_BLOCK)], ksem.at[slot, s])
            vcopy = pltpu.make_async_copy(
                vb_ref.at[vidx_ref[row * CHOSEN + s]],
                values.at[slot, pl.ds(s * KEY_BLOCK, KEY_BLOCK), pl.ds(0, 128)], vsem.at[slot, s])
            if start:
                kcopy.start()
                vcopy.start()
            else:
                kcopy.wait()
                vcopy.wait()

    @pl.when(b == 0)
    def _():
        fetch(0, 0, True)
        for slot in range(2):
            values[slot, :, 128:256] = jnp.ones((values.shape[1], 128), jnp.bfloat16)

    slot = lax.rem(b, 2)
    far = CHOSEN * KEY_BLOCK

    @pl.when(b + 1 < count)
    def _():
        fetch(b + 1, 1 - slot, True)

    fetch(b, slot, False)
    keys[slot, far:, :] = k_ref[...]
    values[slot, far:, 0:128] = v_ref[...]
    all_keys = keys[slot]
    all_values = values[slot]
    lane = lax.broadcasted_iota(jnp.int32, (QUERY_BLOCK, 128), 1)
    first_head = lane < HEAD_DIM
    query_at = lax.broadcasted_iota(jnp.int32, (QUERY_BLOCK, QUERY_BLOCK), 0)
    key_at = lax.broadcasted_iota(jnp.int32, (QUERY_BLOCK, QUERY_BLOCK), 1)
    causal = query_at >= key_at
    bias = bias_ref[0]
    scale = HEAD_DIM ** -0.5 * LOG2E
    mixed = []
    for g in range(4):
        q = q_ref[:, 128 * g : 128 * (g + 1)]
        parts = []
        for n in range(2):
            own = jnp.where(first_head if n == 0 else jnp.logical_not(first_head), q, jnp.zeros_like(q))
            scores = lax.dot_general(own, all_keys, (((1,), (1,)), ((), ())), preferred_element_type=jnp.float32)
            scores_far = scores[:, :far] + bias
            scores_own = jnp.where(causal, scores[:, far:], -jnp.inf)
            top = jnp.maximum(
                jnp.max(scores_far, axis=1, keepdims=True), jnp.max(scores_own, axis=1, keepdims=True))
            weights = jnp.concatenate(
                [jnp.exp2((scores_far - top) * scale).astype(jnp.bfloat16),
                 jnp.exp2((scores_own - top) * scale).astype(jnp.bfloat16)], axis=1)
            summed = jnp.dot(weights, all_values, preferred_element_type=jnp.float32)
            parts.append(summed[:, :128] / summed[:, 128:])
        mixed.append(jnp.where(first_head, parts[0], parts[1]))
    swapped = [pltpu.roll(u, 64, 1) for u in mixed]
    ordered = [
        jnp.where(first_head, mixed[0], swapped[1]),
        jnp.where(first_head, mixed[2], swapped[3]),
        jnp.where(first_head, swapped[0], mixed[1]),
        jnp.where(first_head, swapped[2], mixed[3]),
    ]
    for i in range(4):
        out_ref[:, 128 * i : 128 * (i + 1)] = ordered[i].astype(jnp.bfloat16)


def body(
    tokens, query_weight, key_weight, value_weight, out_weight, norm_gain, chosen_owner, chosen_part
):
    row_data = tokens[0]
    tok_count = row_data.shape[0]
    me = lax.axis_index("kv")
    z, x = me // NX, me % NX
    positions = me * tok_count + jnp.arange(tok_count, dtype=jnp.int32)
    half_dim = HEAD_DIM // 2
    frequency = rope_base ** (-jnp.arange(half_dim, dtype=jnp.float32) / half_dim)
    angles = positions.astype(jnp.float32)[:, None] * frequency
    cosine, sine = jnp.cos(angles), jnp.sin(angles)
    cosine = jnp.concatenate([cosine] * 4, axis=1)
    sine = jnp.concatenate([-sine, sine, -sine, sine], axis=1)
    tile = 256
    queries, keys, values = pl.pallas_call(
        project_kernel,
        grid=(tok_count // tile,),
        in_specs=[
            pl.BlockSpec((tile, D), lambda i: (i, 0)),
            pl.BlockSpec((D, 512), lambda i: (0, 0)),
            pl.BlockSpec((D, 128), lambda i: (0, 0)),
            pl.BlockSpec((D, 128), lambda i: (0, 0)),
            pl.BlockSpec((tile, 128), lambda i: (i, 0)),
            pl.BlockSpec((tile, 128), lambda i: (i, 0)),
        ],
        out_specs=[
            pl.BlockSpec((tile, 512), lambda i: (i, 0)),
            pl.BlockSpec((tile, 128), lambda i: (i, 0)),
            pl.BlockSpec((tile, 128), lambda i: (i, 0)),
        ],
        out_shape=[
            jax.ShapeDtypeStruct((tok_count, 512), jnp.bfloat16),
            jax.ShapeDtypeStruct((tok_count, 128), jnp.bfloat16),
            jax.ShapeDtypeStruct((tok_count, 128), jnp.bfloat16),
        ],
    )(row_data, query_weight, key_weight, value_weight, cosine, sine)

    owners, parts = chosen_owner[0], chosen_part[0]
    row_owner = lax.dynamic_slice_in_dim(owners, z * NX * ROWS, NX * ROWS, 0)
    row_part = lax.dynamic_slice_in_dim(parts, z * NX * ROWS, NX * ROWS, 0)
    everyone = jnp.arange(NZ * NX, dtype=jnp.int32)
    table = jnp.sum(
        jnp.where(row_owner[:, :, None] == everyone, row_part[:, :, None], 0), axis=1
    ).reshape(NX * ROWS * NZ * NX)
    mine_owner = lax.dynamic_slice_in_dim(owners, me * ROWS, ROWS, 0)
    mine_part = lax.dynamic_slice_in_dim(parts, me * ROWS, ROWS, 0)
    valid = mine_owner >= 0
    safe = jnp.maximum(mine_owner, 0)
    slot = (z - safe // NX + NZ) % NZ
    across = (safe % NX - x + NX) % NX
    row = jnp.arange(ROWS, dtype=jnp.int32)[:, None]
    full_at = slot * PARTS + mine_part
    sel_at = 2 * FULL + slot * ROWS + row
    kidx = jnp.where(across == 0, full_at, jnp.where(across == 3, FULL + full_at, jnp.where(across == 1, sel_at, SEL + sel_at)))
    vidx = jnp.where(across == 0, full_at, jnp.where(across == 1, FULL + full_at, jnp.where(across == 3, sel_at, SEL + sel_at)))
    kidx = jnp.where(valid, kidx, 0).reshape(ROWS * CHOSEN)
    vidx = jnp.where(valid, vidx, 0).reshape(ROWS * CHOSEN)
    bias = jnp.where(jnp.repeat(valid, KEY_BLOCK, axis=1), 0.0, -jnp.inf).astype(jnp.float32)[:, None, :]

    vmem = pl.BlockSpec(memory_space=pltpu.VMEM)
    smem = pl.BlockSpec(memory_space=pltpu.SMEM)
    anyspace = pl.BlockSpec(memory_space=pl.ANY)
    pool = jax.ShapeDtypeStruct((BLOCKS, KEY_BLOCK, 128), jnp.bfloat16)
    kb, vb = pl.pallas_call(
        exchange_kernel,
        in_specs=[smem, vmem, vmem],
        out_specs=[vmem, vmem],
        out_shape=[pool, pool],
        scratch_shapes=[
            pltpu.VMEM((PARTS, KEY_BLOCK, 128), jnp.bfloat16),
            pltpu.VMEM((NZ, 4, ROWS, KEY_BLOCK, 128), jnp.bfloat16),
            pltpu.SemaphoreType.DMA((2, NZ // 2, 4)),
            pltpu.SemaphoreType.DMA((2, NZ // 2, 4)),
            pltpu.SemaphoreType.DMA((2,)),
            pltpu.SemaphoreType.DMA((2,)),
            pltpu.SemaphoreType.DMA((NZ, 4)),
            pltpu.SemaphoreType.DMA((NZ, 4)),
        ],
        compiler_params=pltpu.CompilerParams(collective_id=0, has_side_effects=True),
    )(table, keys.reshape(PARTS, KEY_BLOCK, 128), values.reshape(PARTS, KEY_BLOCK, 128))

    mixed_rows = pl.pallas_call(
        attend_kernel,
        grid_spec=pltpu.PrefetchScalarGridSpec(
            num_scalar_prefetch=2,
            grid=(ROWS,),
            in_specs=[
                pl.BlockSpec((1, 1, CHOSEN * KEY_BLOCK), lambda i, a, c: (i, 0, 0)),
                pl.BlockSpec((QUERY_BLOCK, 512), lambda i, a, c: (i, 0)),
                pl.BlockSpec((QUERY_BLOCK, 128), lambda i, a, c: (i, 0)),
                pl.BlockSpec((QUERY_BLOCK, 128), lambda i, a, c: (i, 0)),
                anyspace,
                anyspace,
            ],
            out_specs=pl.BlockSpec((QUERY_BLOCK, 512), lambda i, a, c: (i, 0)),
            scratch_shapes=[
                pltpu.VMEM((2, CHOSEN * KEY_BLOCK + QUERY_BLOCK, 128), jnp.bfloat16),
                pltpu.VMEM((2, CHOSEN * KEY_BLOCK + QUERY_BLOCK, 256), jnp.bfloat16),
                pltpu.SemaphoreType.DMA((2, CHOSEN)),
                pltpu.SemaphoreType.DMA((2, CHOSEN)),
            ],
        ),
        out_shape=jax.ShapeDtypeStruct((tok_count, 512), jnp.bfloat16),
    )(kidx, vidx, bias, queries, keys, values, kb, vb)

    terms = jnp.dot(mixed_rows, out_weight, preferred_element_type=jnp.float32)
    projected = summed_on_arrival(terms.astype(jnp.bfloat16), "tp", 1)
    row_total = lax.psum(jnp.sum(projected * projected, axis=1), "tp")
    scale_rows = lax.rsqrt(row_total / D + norm_eps)
    result = (projected * scale_rows[:, None] * norm_gain[None, :]).astype(jnp.bfloat16)
    return result[None]


def solution(mesh):
    placed = (
        P("dp", "kv", None),
        P(None, "tp"),
        P(None, "tp"),
        P(None, "tp"),
        P("tp", None),
        P("tp"),
        P("dp", None, None),
        P("dp", None, None),
    )
    return jax.shard_map(
        body, mesh=mesh, in_specs=placed, out_specs=P("dp", "kv", "tp"), check_vma=False
    )
```

```python
import jax
import jax.numpy as jnp
from jax import lax
from jax.experimental import pallas as pl
from jax.experimental.pallas import tpu as pltpu
from jax.sharding import PartitionSpec as P

D = 2048
HEAD_DIM = 64
QUERY_BLOCK = 128
KEY_BLOCK = 64
NZ = 8
NX = 4
ROWS = 6
PARTS = 12
CHOSEN = 16
FULL = NZ * PARTS
SEL = NZ * ROWS
BLOCKS = 2 * FULL + 2 * SEL
rope_base = 10000.0
norm_eps = 1e-06
MESH = pl.DeviceIdType.MESH
LOG2E = 1.4426950408889634


def split_up(x, dim, count):
    before, after = (x.shape[:dim], x.shape[dim + 1 :])
    return jnp.moveaxis(x.reshape(*before, count, -1, *after), dim, 0)


def summed_on_arrival(x, axis, dim):
    count = lax.axis_size(axis)
    blocks = lax.all_to_all(split_up(x, dim, count), axis, 0, 0, tiled=True)
    return jnp.sum(blocks.astype(jnp.float32), axis=0)


def turned(u, cosine, sine, low_half):
    other = jnp.where(low_half, pltpu.roll(u, 96, 1), pltpu.roll(u, 32, 1))
    return u * cosine + other * sine


def project_kernel(z_ref, x_ref, wk_ref, wv_ref, cos_ref, sin_ref, owner_ref, part_ref, k_ref, v_ref, t_ref):
    x = x_ref[...]
    cosine, sine = cos_ref[...], sin_ref[...]
    lane = lax.broadcasted_iota(jnp.int32, cosine.shape, 1)
    low_half = (lane % HEAD_DIM) < HEAD_DIM // 2
    keys = jnp.dot(x, wk_ref[...], preferred_element_type=jnp.float32)
    k_ref[...] = turned(keys, cosine, sine, low_half).astype(jnp.bfloat16)
    v_ref[...] = jnp.dot(x, wv_ref[...], preferred_element_type=jnp.float32).astype(jnp.bfloat16)

    @pl.when(pl.program_id(0) == 0)
    def _():
        owner, part = owner_ref[...], part_ref[...]
        owner_at = lax.broadcasted_iota(jnp.int32, t_ref.shape, 1)
        table = jnp.full(t_ref.shape, -1, jnp.int32)
        for s in range(CHOSEN):
            table = jnp.where(owner[:, s : s + 1] == owner_at, part[:, s : s + 1], table)
        t_ref[...] = table


NEAR = (0, 1, 2, 6, 7)
FAR = (3, 4, 5)
WIDTH = 512
SUMS = 80


def exchange_kernel(
    t_ref, k_ref, v_ref, cos_ref, sin_ref, x_hbm, wq_hbm, out_ref,
    x_vm, wq_vm, qz, top_ref, acc_ref, whole,
    own_k, own_v, nb_k, nb_v,
    self_k, self_v, selfn_k, selfn_v,
    to_left_k, to_right_v, to_right_k, to_left_v, opp_k, opp_v, near_k, near_v,
    from_right_k, from_left_v, from_left_k, from_right_v, across_k, across_v, relay_k, relay_v,
    load_sem, zsend, zrecv, nsend, nrecv, ssend, srecv, rsend, rrecv,
):
    me = lax.axis_index("kv")
    z, x = me // NX, me % NX
    up = ((z + 1) % NZ) * NX + x
    down = ((z + NZ - 1) % NZ) * NX + x
    xr, xl, xo = (x + 1) % NX, (x + NX - 1) % NX, (x + 2) % NX
    right = z * NX + xr
    left = z * NX + xl
    load_x = pltpu.make_async_copy(x_hbm, x_vm, load_sem.at[0])
    load_w = pltpu.make_async_copy(wq_hbm, wq_vm, load_sem.at[1])
    load_x.start()
    load_w.start()
    barrier = pltpu.get_barrier_semaphore()
    for peer in (up, down, right, left):
        pl.semaphore_signal(barrier, inc=1, device_id={"kv": peer}, device_id_type=MESH)
    pl.semaphore_wait(barrier, 4)
    sent = []

    def send(src, dst, ssem, rsem, peer):
        copy = pltpu.make_async_remote_copy(
            src_ref=src, dst_ref=dst, send_sem=ssem, recv_sem=rsem,
            device_id={"kv": peer}, device_id_type=MESH,
        )
        copy.start()
        sent.append(copy)
        return copy

    def chunk(kind, slot):
        if kind < 2:
            if slot == 0:
                return (k_ref, v_ref)[kind]
            return (own_k, own_v)[kind].at[slot - 1]
        return (nb_k, nb_v)[kind - 2].at[NEAR.index(slot)]

    arrivals = {}

    def forward(kind, step):
        for direction in range(2):
            if step == NZ // 2 and kind % 2 != direction:
                continue
            new = step if direction == 0 else NZ - step
            old = (step - 1) if direction == 0 else (NZ - step + 1) % NZ
            arrivals[direction, step, kind] = send(
                chunk(kind, old), chunk(kind, new), zsend.at[direction, step - 1, kind],
                zrecv.at[direction, step - 1, kind], up if direction == 0 else down,
            )

    def owner_of(slot, column):
        return ((z + NZ - slot) % NZ) * NX + column

    def choose(target, dest_x, owner):
        for r in range(ROWS):
            part = t_ref[dest_x * ROWS + r, owner]
            target[r] = whole[jnp.maximum(part, 0)]

    got = {}

    def pick(kind, slot):
        is_v = kind % 2
        whole[...] = chunk(kind, slot)[...]
        jobs = []
        if kind < 2:
            owner = owner_of(slot, x)
            stage = (to_left_k, to_right_v)[is_v].at[slot]
            choose(stage, (xl, xr)[is_v], owner)
            jobs.append((stage, (from_right_k, from_left_v)[is_v].at[slot], 0, (left, right)[is_v]))
            if slot in FAR:
                at = FAR.index(slot)
                stage = (to_right_k, to_left_v)[is_v].at[at]
                choose(stage, (xr, xl)[is_v], owner)
                jobs.append((stage, (from_left_k, from_right_v)[is_v].at[at], 1, (right, left)[is_v]))
                stage = (opp_k, opp_v)[is_v].at[at]
                choose(stage, xo, owner)
                jobs.append((stage, (relay_k, relay_v)[is_v].at[at], 2, (right, left)[is_v]))
            choose((self_k, self_v)[is_v].at[slot], x, owner)
        else:
            owner = owner_of(slot, (xl, xr)[is_v])
            at = NEAR.index(slot)
            stage = (near_k, near_v)[is_v].at[at]
            choose(stage, (xr, xl)[is_v], owner)
            jobs.append((stage, (across_k, across_v)[is_v].at[slot], 3, (right, left)[is_v]))
            choose((selfn_k, selfn_v)[is_v].at[at], x, owner)
        for stage, place, which, peer in jobs:
            got[is_v, slot, which] = send(
                stage, place, ssend.at[is_v, slot, which], srecv.at[is_v, slot, which], peer)

    def pass_on(is_v, slot):
        at = FAR.index(slot)
        got[is_v, slot, 2].wait_recv()
        got[is_v, slot, 3] = send(
            (relay_k, relay_v)[is_v].at[at], (across_k, across_v)[is_v].at[slot],
            rsend.at[is_v, at], rrecv.at[is_v, at], (right, left)[is_v])

    def arrive(kind, step, onward):
        slots = []
        for direction in range(2):
            if (direction, step, kind) in arrivals:
                arrivals[direction, step, kind].wait_recv()
                slots.append(step if direction == 0 else NZ - step)
        if onward:
            forward(kind, step + 1)
        for slot in slots:
            pick(kind, slot)

    def candidate(slot, column):
        is_far = slot in FAR
        if column == "own":
            return self_k.at[slot], self_v.at[slot], owner_of(slot, x)
        if column == "right":
            values = from_right_v.at[FAR.index(slot)] if is_far else selfn_v.at[NEAR.index(slot)]
            return from_right_k.at[slot], values, owner_of(slot, xr)
        if column == "left":
            keys = from_left_k.at[FAR.index(slot)] if is_far else selfn_k.at[NEAR.index(slot)]
            return keys, from_left_v.at[slot], owner_of(slot, xl)
        return across_k.at[slot], across_v.at[slot], owner_of(slot, xo)

    def ready(slot):
        for is_v in range(2):
            got[is_v, slot, 0].wait_recv()
            if slot in FAR:
                got[is_v, slot, 1].wait_recv()
            got[is_v, slot, 3].wait_recv()

    scale = HEAD_DIM ** -0.5 * LOG2E

    def attend(names, first, last):
        blocks = [candidate(slot, column) for slot, column in names]

        def one_row(r, carry):
            keys = [b[0][r] for b in blocks]
            values = [b[1][r] for b in blocks]
            away = []
            for b in blocks:
                part = t_ref[x * ROWS + r, b[2]]
                away.append(jnp.where(part < 0, jnp.float32(jnp.inf), jnp.float32(0)))
            if first:
                for half in range(2):
                    keys.append(k_ref[2 * r + half])
                    values.append(v_ref[2 * r + half])
            all_keys = jnp.concatenate(keys, axis=0)
            turned_values = jnp.concatenate(values, axis=0).T
            far = len(blocks) * KEY_BLOCK
            count = all_keys.shape[0]
            ones = jnp.ones((SUMS - HEAD_DIM, count), jnp.bfloat16)
            for n in range(2):
                scores = lax.dot_general(
                    all_keys, qz[r, n], (((1,), (1,)), ((), ())), preferred_element_type=jnp.float32)
                pieces = [scores[KEY_BLOCK * i : KEY_BLOCK * (i + 1)] for i in range(len(blocks))]
                top = None if first else top_ref[r, n]
                old = top
                for piece, gone in zip(pieces, away):
                    peak = jnp.max(piece, axis=0, keepdims=True) - gone
                    top = peak if top is None else jnp.maximum(top, peak)
                if first:
                    key_at = lax.broadcasted_iota(jnp.int32, (QUERY_BLOCK, WIDTH), 0)
                    query_at = lax.broadcasted_iota(jnp.int32, (QUERY_BLOCK, WIDTH), 1) % QUERY_BLOCK
                    own = jnp.where(key_at <= query_at, scores[far:], -jnp.inf)
                    top = jnp.maximum(top, jnp.max(own, axis=0, keepdims=True))
                weights = [
                    jnp.exp2((piece - (top + gone)) * scale).astype(jnp.bfloat16)
                    for piece, gone in zip(pieces, away)
                ]
                if first:
                    weights.append(jnp.exp2((own - top) * scale).astype(jnp.bfloat16))
                left_side = jnp.concatenate(
                    [turned_values[HEAD_DIM * n : HEAD_DIM * (n + 1)], ones], axis=0)
                total = jnp.dot(
                    left_side, jnp.concatenate(weights, axis=0), preferred_element_type=jnp.float32)
                if not first:
                    total = total + acc_ref[r, n] * jnp.exp2((old - top) * scale)
                if not last:
                    top_ref[r, n] = top
                    acc_ref[r, n] = total
                else:
                    mixed = total[:HEAD_DIM] / total[HEAD_DIM : HEAD_DIM + 1]
                    at = pl.ds(pl.multiple_of(r * QUERY_BLOCK, QUERY_BLOCK), QUERY_BLOCK)
                    for p in range(2):
                        pair = jnp.concatenate(
                            [mixed[:, 256 * p : 256 * p + 128], mixed[:, 256 * p + 128 : 256 * p + 256]],
                            axis=0)
                        column = 256 * n + 128 * p
                        out_ref[at, column : column + 128] = pair.T.astype(jnp.bfloat16)
            return carry

        lax.fori_loop(0, ROWS, one_row, 0)

    def project_queries():
        load_x.wait()
        load_w.wait()

        def one_row(r, carry):
            at = pl.ds(pl.multiple_of(r * QUERY_BLOCK, QUERY_BLOCK), QUERY_BLOCK)
            q = jnp.dot(x_vm[at, :], wq_vm[...], preferred_element_type=jnp.float32)
            cosine, sine = cos_ref[at, :], sin_ref[at, :]
            lane = lax.broadcasted_iota(jnp.int32, cosine.shape, 1)
            low_half = (lane % HEAD_DIM) < HEAD_DIM // 2
            for n in range(2):
                mine = (lane < HEAD_DIM) if n == 0 else (lane >= HEAD_DIM)
                for p in range(2):
                    column = 256 * n + 128 * p
                    pair = turned(q[:, column : column + 128], cosine, sine, low_half)
                    other = pltpu.roll(pair, 64, 1)
                    for g in range(2):
                        head = pair if g == n else other
                        place = (2 * p + g) * QUERY_BLOCK
                        qz[r, n, place : place + QUERY_BLOCK] = jnp.where(mine, head, 0.0).astype(jnp.bfloat16)
            return carry

        lax.fori_loop(0, ROWS, one_row, 0)

    forward(0, 1)
    forward(1, 1)
    near0 = [
        send(k_ref, chunk(2, 0), nsend.at[0], nrecv.at[0], right),
        send(v_ref, chunk(3, 0), nsend.at[1], nrecv.at[1], left),
    ]
    pick(0, 0)
    pick(1, 0)
    project_queries()
    arrive(0, 1, True)
    for kind in (2, 3):
        near0[kind - 2].wait_recv()
        pick(kind, 0)
    arrive(1, 1, True)
    arrive(0, 2, True)
    ready(0)
    arrive(1, 2, True)
    attend([(0, c) for c in ("own", "right", "left", "across")], True, False)
    arrive(0, 3, True)
    arrive(1, 3, True)
    forward(2, 1)
    forward(3, 1)
    arrive(0, 4, False)
    pass_on(0, 3)
    pass_on(0, 5)
    arrive(1, 4, False)
    pass_on(1, 3)
    pass_on(1, 5)
    attend([(s, "own") for s in range(1, NZ)], False, False)
    arrive(2, 1, True)
    pass_on(0, 4)
    arrive(3, 1, True)
    pass_on(1, 4)
    for slot in FAR:
        ready(slot)
    attend([(s, c) for s in FAR for c in ("right", "left", "across")], False, False)
    arrive(2, 2, False)
    ready(1)
    ready(7)
    arrive(3, 2, False)
    attend([(s, c) for s in (1, 7) for c in ("right", "left", "across")], False, False)
    ready(2)
    ready(6)
    attend([(s, c) for s in (2, 6) for c in ("right", "left", "across")], False, True)
    for copy in sent:
        copy.wait_send()


def body(
    tokens, query_weight, key_weight, value_weight, out_weight, norm_gain, chosen_owner, chosen_part
):
    row_data = tokens[0]
    tok_count = row_data.shape[0]
    me = lax.axis_index("kv")
    z, x = me // NX, me % NX
    positions = me * tok_count + jnp.arange(tok_count, dtype=jnp.int32)
    half_dim = HEAD_DIM // 2
    lane = jnp.arange(128, dtype=jnp.int32)
    frequency = rope_base ** (-(lane % half_dim).astype(jnp.float32) / half_dim)
    angles = positions.astype(jnp.float32)[:, None] * frequency
    cosine = jnp.cos(angles)
    sine = jnp.sin(angles) * jnp.where(lane % HEAD_DIM < half_dim, -1.0, 1.0).astype(jnp.float32)
    tile = 256
    around = NX * ROWS
    keys, values, table = pl.pallas_call(
        project_kernel,
        grid_spec=pltpu.PrefetchScalarGridSpec(
            num_scalar_prefetch=1,
            grid=(tok_count // tile,),
            in_specs=[
                pl.BlockSpec((tile, D), lambda i, at: (i, 0)),
                pl.BlockSpec((D, 128), lambda i, at: (0, 0)),
                pl.BlockSpec((D, 128), lambda i, at: (0, 0)),
                pl.BlockSpec((tile, 128), lambda i, at: (i, 0)),
                pl.BlockSpec((tile, 128), lambda i, at: (i, 0)),
                pl.BlockSpec((around, CHOSEN), lambda i, at: (at[0], 0)),
                pl.BlockSpec((around, CHOSEN), lambda i, at: (at[0], 0)),
            ],
            out_specs=[
                pl.BlockSpec((tile, 128), lambda i, at: (i, 0)),
                pl.BlockSpec((tile, 128), lambda i, at: (i, 0)),
                pl.BlockSpec((around, NZ * NX), lambda i, at: (0, 0)),
            ],
        ),
        out_shape=[
            jax.ShapeDtypeStruct((tok_count, 128), jnp.bfloat16),
            jax.ShapeDtypeStruct((tok_count, 128), jnp.bfloat16),
            jax.ShapeDtypeStruct((around, NZ * NX), jnp.int32),
        ],
    )(z.reshape(1), row_data, key_weight, value_weight, cosine, sine, chosen_owner[0], chosen_part[0])

    vmem = pl.BlockSpec(memory_space=pltpu.VMEM)
    smem = pl.BlockSpec(memory_space=pltpu.SMEM)
    anyspace = pl.BlockSpec(memory_space=pl.ANY)

    def chunks(count):
        return pltpu.VMEM((count, PARTS, KEY_BLOCK, 128), jnp.bfloat16)

    def picks(count):
        return pltpu.VMEM((count, ROWS, KEY_BLOCK, 128), jnp.bfloat16)

    def sems(*shape):
        return pltpu.SemaphoreType.DMA(shape)

    mixed_rows = pl.pallas_call(
        exchange_kernel,
        in_specs=[smem, vmem, vmem, vmem, vmem, anyspace, anyspace],
        out_specs=vmem,
        out_shape=jax.ShapeDtypeStruct((tok_count, WIDTH), jnp.bfloat16),
        scratch_shapes=[
            pltpu.VMEM((tok_count, D), jnp.bfloat16),
            pltpu.VMEM((D, WIDTH), jnp.bfloat16),
            pltpu.VMEM((ROWS, 2, WIDTH, 128), jnp.bfloat16),
            pltpu.VMEM((ROWS, 2, 1, WIDTH), jnp.float32),
            pltpu.VMEM((ROWS, 2, SUMS, WIDTH), jnp.float32),
            pltpu.VMEM((PARTS, KEY_BLOCK, 128), jnp.bfloat16),
            chunks(7), chunks(7), chunks(5), chunks(5),
            picks(8), picks(8), picks(5), picks(5),
            picks(8), picks(8), picks(3), picks(3), picks(3), picks(3), picks(5), picks(5),
            picks(8), picks(8), picks(3), picks(3), picks(8), picks(8), picks(3), picks(3),
            sems(2),
            sems(2, 4, 4), sems(2, 4, 4),
            sems(2), sems(2),
            sems(2, 8, 4), sems(2, 8, 4),
            sems(2, 3), sems(2, 3),
        ],
        compiler_params=pltpu.CompilerParams(collective_id=0, has_side_effects=True),
    )(table, keys.reshape(PARTS, KEY_BLOCK, 128), values.reshape(PARTS, KEY_BLOCK, 128),
      cosine, sine, row_data, query_weight)

    terms = jnp.dot(mixed_rows, out_weight, preferred_element_type=jnp.float32)
    projected = summed_on_arrival(terms.astype(jnp.bfloat16), "tp", 1)
    row_total = lax.psum(jnp.sum(projected * projected, axis=1), "tp")
    scale_rows = lax.rsqrt(row_total / D + norm_eps)
    result = (projected * scale_rows[:, None] * norm_gain[None, :]).astype(jnp.bfloat16)
    return result[None]


def solution(mesh):
    placed = (
        P("dp", "kv", None),
        P(None, "tp"),
        P(None, "tp"),
        P(None, "tp"),
        P("tp", None),
        P("tp"),
        P("dp", None, None),
        P("dp", None, None),
    )
    return jax.shard_map(
        body, mesh=mesh, in_specs=placed, out_specs=P("dp", "kv", "tp"), check_vma=False
    )
```

```python
import jax
import jax.numpy as jnp
from jax import lax
from jax.experimental import pallas as pl
from jax.experimental.pallas import tpu as pltpu
from jax.sharding import PartitionSpec as P

D = 2048
HEAD_DIM = 64
QUERY_BLOCK = 128
KEY_BLOCK = 64
NZ = 8
NX = 4
ROWS = 6
PARTS = 12
CHOSEN = 16
FULL = NZ * PARTS
SEL = NZ * ROWS
BLOCKS = 2 * FULL + 2 * SEL
rope_base = 10000.0
norm_eps = 1e-06
MESH = pl.DeviceIdType.MESH
LOG2E = 1.4426950408889634


def split_up(x, dim, count):
    before, after = (x.shape[:dim], x.shape[dim + 1 :])
    return jnp.moveaxis(x.reshape(*before, count, -1, *after), dim, 0)


def summed_on_arrival(x, axis, dim):
    count = lax.axis_size(axis)
    blocks = lax.all_to_all(split_up(x, dim, count), axis, 0, 0, tiled=True)
    return jnp.sum(blocks.astype(jnp.float32), axis=0)


def turned(u, cosine, sine, low_half):
    other = jnp.where(low_half, pltpu.roll(u, 96, 1), pltpu.roll(u, 32, 1))
    return u * cosine + other * sine


def project_kernel(x_ref, wk_ref, wv_ref, cos_ref, sin_ref, owner_ref, part_ref, k_ref, v_ref, t_ref):
    x = x_ref[...]
    cosine, sine = cos_ref[...], sin_ref[...]
    lane = lax.broadcasted_iota(jnp.int32, cosine.shape, 1)
    low_half = (lane % HEAD_DIM) < HEAD_DIM // 2
    keys = jnp.dot(x, wk_ref[...], preferred_element_type=jnp.float32)
    k_ref[...] = turned(keys, cosine, sine, low_half).astype(jnp.bfloat16)
    v_ref[...] = jnp.dot(x, wv_ref[...], preferred_element_type=jnp.float32).astype(jnp.bfloat16)

    @pl.when(pl.program_id(0) == 0)
    def _():
        owner, part = owner_ref[...], part_ref[...]
        owner_at = lax.broadcasted_iota(jnp.int32, t_ref.shape, 0)
        table = jnp.full(t_ref.shape, -1, jnp.int32)
        for s in range(CHOSEN):
            table = jnp.where(owner[s : s + 1] == owner_at, part[s : s + 1], table)
        t_ref[...] = table


NEAR = ((0, 1, 2, 5, 6, 7), (0, 1, 2, 3, 6, 7))
FAR = ((3, 4), (4, 5))
WIDTH = 512
SUMS = 80


def exchange_kernel(
    t_ref, k_ref, v_ref, cos_ref, sin_ref, x_hbm, wq_hbm, out_ref,
    x_vm, wq_vm, qz, top_ref, acc_ref, whole,
    own_k, own_v, nb_k, nb_v,
    self_k, self_v, selfn_k, selfn_v,
    to_left_k, to_right_v, to_right_k, to_left_v, opp_k, opp_v, near_k, near_v,
    from_right_k, from_left_v, from_left_k, from_right_v, across_k, across_v, relay_k, relay_v,
    load_sem, zsend, zrecv, nsend, nrecv, ssend, srecv, rsend, rrecv,
):
    me = lax.axis_index("kv")
    z, x = me // NX, me % NX
    up = ((z + 1) % NZ) * NX + x
    down = ((z + NZ - 1) % NZ) * NX + x
    xr, xl, xo = (x + 1) % NX, (x + NX - 1) % NX, (x + 2) % NX
    right = z * NX + xr
    left = z * NX + xl
    load_x = pltpu.make_async_copy(x_hbm, x_vm, load_sem.at[0])
    load_w = pltpu.make_async_copy(wq_hbm, wq_vm, load_sem.at[1])
    load_x.start()
    load_w.start()
    barrier = pltpu.get_barrier_semaphore()
    for peer in (up, down, right, left):
        pl.semaphore_signal(barrier, inc=1, device_id={"kv": peer}, device_id_type=MESH)
    pl.semaphore_wait(barrier, 4)
    sent = []

    def send(src, dst, ssem, rsem, peer):
        copy = pltpu.make_async_remote_copy(
            src_ref=src, dst_ref=dst, send_sem=ssem, recv_sem=rsem,
            device_id={"kv": peer}, device_id_type=MESH,
        )
        copy.start()
        sent.append(copy)
        return copy

    def chunk(kind, slot):
        if kind < 2:
            if slot == 0:
                return (k_ref, v_ref)[kind]
            return (own_k, own_v)[kind].at[slot - 1]
        return (nb_k, nb_v)[kind - 2].at[NEAR[kind - 2].index(slot)]

    arrivals = {}

    def forward(kind, step, directions=(0, 1)):
        for direction in directions:
            if step == NZ // 2 and kind % 2 != direction:
                continue
            if kind >= 2 and step == 3 and kind % 2 == direction:
                continue
            new = step if direction == 0 else NZ - step
            old = (step - 1) if direction == 0 else (NZ - step + 1) % NZ
            arrivals[direction, step, kind] = send(
                chunk(kind, old), chunk(kind, new), zsend.at[direction, step - 1, kind],
                zrecv.at[direction, step - 1, kind], up if direction == 0 else down,
            )

    def owner_of(slot, column):
        return ((z + NZ - slot) % NZ) * NX + column

    def choose(target, dest_x, owner):
        for r in range(ROWS):
            part = t_ref[owner, (z * NX + dest_x) * ROWS + r]
            target[r] = whole[jnp.maximum(part, 0)]

    got = {}

    def pick(kind, slot):
        is_v = kind % 2
        whole[...] = chunk(kind, slot)[...]
        jobs = []
        if kind < 2:
            owner = owner_of(slot, x)
            stage = (to_left_k, to_right_v)[is_v].at[slot]
            choose(stage, (xl, xr)[is_v], owner)
            jobs.append((stage, (from_right_k, from_left_v)[is_v].at[slot], 0, (left, right)[is_v]))
            if slot in FAR[is_v]:
                at = FAR[is_v].index(slot)
                stage = (to_right_k, to_left_v)[is_v].at[at]
                choose(stage, (xr, xl)[is_v], owner)
                jobs.append((stage, (from_left_k, from_right_v)[is_v].at[at], 1, (right, left)[is_v]))
                stage = (opp_k, opp_v)[is_v].at[at]
                choose(stage, xo, owner)
                jobs.append((stage, (relay_k, relay_v)[is_v].at[at], 2, (right, left)[is_v]))
            choose((self_k, self_v)[is_v].at[slot], x, owner)
        else:
            owner = owner_of(slot, (xl, xr)[is_v])
            at = NEAR[is_v].index(slot)
            stage = (near_k, near_v)[is_v].at[at]
            choose(stage, (xr, xl)[is_v], owner)
            jobs.append((stage, (across_k, across_v)[is_v].at[slot], 3, (right, left)[is_v]))
            choose((selfn_k, selfn_v)[is_v].at[at], x, owner)
        for stage, place, which, peer in jobs:
            got[is_v, slot, which] = send(
                stage, place, ssend.at[is_v, slot, which], srecv.at[is_v, slot, which], peer)

    def pass_on(is_v, slot):
        at = FAR[is_v].index(slot)
        got[is_v, slot, 2].wait_recv()
        got[is_v, slot, 3] = send(
            (relay_k, relay_v)[is_v].at[at], (across_k, across_v)[is_v].at[slot],
            rsend.at[is_v, at], rrecv.at[is_v, at], (right, left)[is_v])

    def arrive(kind, step, onward, directions=(0, 1)):
        slots = []
        for direction in directions:
            if (direction, step, kind) in arrivals:
                arrivals[direction, step, kind].wait_recv()
                slots.append(step if direction == 0 else NZ - step)
                if onward:
                    forward(kind, step + 1, (direction,))
        for slot in slots:
            pick(kind, slot)

    def candidate(slot, column):
        if column == "own":
            return self_k.at[slot], self_v.at[slot], owner_of(slot, x)
        if column == "right":
            values = (
                from_right_v.at[FAR[1].index(slot)] if slot in FAR[1] else selfn_v.at[NEAR[1].index(slot)])
            return from_right_k.at[slot], values, owner_of(slot, xr)
        if column == "left":
            keys = from_left_k.at[FAR[0].index(slot)] if slot in FAR[0] else selfn_k.at[NEAR[0].index(slot)]
            return keys, from_left_v.at[slot], owner_of(slot, xl)
        return across_k.at[slot], across_v.at[slot], owner_of(slot, xo)

    waited = set()

    def ready(names):
        for slot, column in names:
            if column == "own":
                continue
            for is_v in range(2):
                if column == "across":
                    which = 3
                elif (column == "right") == (is_v == 0):
                    which = 0
                elif slot in FAR[is_v]:
                    which = 1
                else:
                    continue
                if (is_v, slot, which) not in waited:
                    waited.add((is_v, slot, which))
                    got[is_v, slot, which].wait_recv()

    scale = HEAD_DIM ** -0.5 * LOG2E

    def attend(names, first, last):
        ready(names)
        blocks = [candidate(slot, column) for slot, column in names]

        def one_row(r, carry):
            keys = [b[0][r] for b in blocks]
            values = [b[1][r] for b in blocks]
            away = []
            for b in blocks:
                part = t_ref[b[2], me * ROWS + r]
                away.append(jnp.where(part < 0, jnp.float32(jnp.inf), jnp.float32(0)))
            if first:
                for half in range(2):
                    keys.append(k_ref[2 * r + half])
                    values.append(v_ref[2 * r + half])
            all_keys = jnp.concatenate(keys, axis=0)
            turned_values = jnp.concatenate(values, axis=0).T
            far = len(blocks) * KEY_BLOCK
            count = all_keys.shape[0]
            ones = jnp.ones((SUMS - HEAD_DIM, count), jnp.bfloat16)
            for n in range(2):
                scores = jnp.dot(all_keys, qz[r, n], preferred_element_type=jnp.float32)
                pieces = [scores[KEY_BLOCK * i : KEY_BLOCK * (i + 1)] for i in range(len(blocks))]
                top = None if first else top_ref[r, n]
                old = top
                for piece, gone in zip(pieces, away):
                    peak = jnp.max(piece, axis=0, keepdims=True) - gone
                    top = peak if top is None else jnp.maximum(top, peak)
                if first:
                    key_at = lax.broadcasted_iota(jnp.int32, (QUERY_BLOCK, WIDTH), 0)
                    query_at = lax.broadcasted_iota(jnp.int32, (QUERY_BLOCK, WIDTH), 1) % QUERY_BLOCK
                    own = jnp.where(key_at <= query_at, scores[far:], -jnp.inf)
                    top = jnp.maximum(top, jnp.max(own, axis=0, keepdims=True))
                weights = [
                    jnp.exp2((piece - (top + gone)) * scale).astype(jnp.bfloat16)
                    for piece, gone in zip(pieces, away)
                ]
                if first:
                    weights.append(jnp.exp2((own - top) * scale).astype(jnp.bfloat16))
                left_side = jnp.concatenate(
                    [turned_values[HEAD_DIM * n : HEAD_DIM * (n + 1)], ones], axis=0)
                total = jnp.dot(
                    left_side, jnp.concatenate(weights, axis=0), preferred_element_type=jnp.float32)
                if not first:
                    total = total + acc_ref[r, n] * jnp.exp2((old - top) * scale)
                if not last:
                    top_ref[r, n] = top
                    acc_ref[r, n] = total
                else:
                    mixed = total[:HEAD_DIM] / total[HEAD_DIM : HEAD_DIM + 1]
                    at = pl.ds(pl.multiple_of(r * QUERY_BLOCK, QUERY_BLOCK), QUERY_BLOCK)
                    for p in range(2):
                        pair = jnp.concatenate(
                            [mixed[:, 256 * p : 256 * p + 128], mixed[:, 256 * p + 128 : 256 * p + 256]],
                            axis=0)
                        column = 256 * n + 128 * p
                        out_ref[at, column : column + 128] = pair.T.astype(jnp.bfloat16)
            return carry

        lax.fori_loop(0, ROWS, one_row, 0, unroll=2)

    def project_queries():
        load_x.wait()
        load_w.wait()

        def one_row(r, carry):
            at = pl.ds(pl.multiple_of(r * QUERY_BLOCK, QUERY_BLOCK), QUERY_BLOCK)
            q = jnp.dot(x_vm[at, :], wq_vm[...], preferred_element_type=jnp.float32)
            cosine, sine = cos_ref[at, :], sin_ref[at, :]
            lane = lax.broadcasted_iota(jnp.int32, cosine.shape, 1)
            low_half = (lane % HEAD_DIM) < HEAD_DIM // 2
            for n in range(2):
                for p in range(2):
                    column = 256 * n + 128 * p
                    pair = turned(q[:, column : column + 128], cosine, sine, low_half).T.astype(jnp.bfloat16)
                    for g in range(2):
                        head = pair[HEAD_DIM * g : HEAD_DIM * (g + 1)]
                        place = (2 * p + g) * QUERY_BLOCK
                        qz[r, n, HEAD_DIM * n : HEAD_DIM * (n + 1), place : place + QUERY_BLOCK] = head
                        qz[r, n, HEAD_DIM * (1 - n) : HEAD_DIM * (2 - n), place : place + QUERY_BLOCK] = (
                            jnp.zeros_like(head))
            return carry

        lax.fori_loop(0, ROWS, one_row, 0)

    others = ("right", "left", "across")
    forward(0, 1)
    forward(1, 1)
    near0 = [
        send(k_ref, chunk(2, 0), nsend.at[0], nrecv.at[0], right),
        send(v_ref, chunk(3, 0), nsend.at[1], nrecv.at[1], left),
    ]
    pick(0, 0)
    pick(1, 0)
    project_queries()
    arrive(0, 1, True)
    for kind in (2, 3):
        near0[kind - 2].wait_recv()
        pick(kind, 0)
    arrive(1, 1, True)
    attend([(0, c) for c in ("own",) + others], True, False)
    arrive(0, 2, True)
    arrive(1, 2, True)
    attend([(s, "own") for s in (1, 7, 2, 6)], False, False)
    arrive(0, 3, True)
    forward(3, 1, (0,))
    forward(2, 1, (1,))
    arrive(1, 3, True)
    forward(2, 1, (0,))
    forward(3, 1, (1,))
    attend([(3, "own"), (5, "own")], False, False)
    arrive(0, 4, False)
    arrive(3, 1, True, (0,))
    arrive(2, 1, True, (1,))
    pass_on(0, 3)
    arrive(1, 4, False)
    pass_on(1, 5)
    attend([(4, "own"), (3, "left"), (5, "right")], False, False)
    arrive(2, 1, True, (0,))
    arrive(3, 1, True, (1,))
    pass_on(0, 4)
    pass_on(1, 4)
    arrive(3, 2, True, (0,))
    arrive(2, 2, True, (1,))
    attend([(4, c) for c in others], False, False)
    arrive(2, 2, False, (0,))
    arrive(3, 2, False, (1,))
    attend([(s, c) for s in (1, 7) for c in others], False, False)
    arrive(3, 3, False, (0,))
    arrive(2, 3, False, (1,))
    attend([(s, c) for s in (2, 6) for c in others], False, False)
    attend([(3, "right"), (3, "across"), (5, "left"), (5, "across")], False, True)
    for copy in sent:
        copy.wait_send()


def body(
    tokens, query_weight, key_weight, value_weight, out_weight, norm_gain, chosen_owner, chosen_part
):
    row_data = tokens[0]
    tok_count = row_data.shape[0]
    me = lax.axis_index("kv")
    z, x = me // NX, me % NX
    positions = me * tok_count + jnp.arange(tok_count, dtype=jnp.int32)
    half_dim = HEAD_DIM // 2
    lane = jnp.arange(128, dtype=jnp.int32)
    frequency = rope_base ** (-(lane % half_dim).astype(jnp.float32) / half_dim)
    angles = positions.astype(jnp.float32)[:, None] * frequency
    cosine = jnp.cos(angles)
    sine = jnp.sin(angles) * jnp.where(lane % HEAD_DIM < half_dim, -1.0, 1.0).astype(jnp.float32)
    tile = 256
    qblocks = chosen_owner.shape[1]
    keys, values, table = pl.pallas_call(
        project_kernel,
        grid_spec=pl.GridSpec(
            grid=(tok_count // tile,),
            in_specs=[
                pl.BlockSpec((tile, D), lambda i: (i, 0)),
                pl.BlockSpec((D, 128), lambda i: (0, 0)),
                pl.BlockSpec((D, 128), lambda i: (0, 0)),
                pl.BlockSpec((tile, 128), lambda i: (i, 0)),
                pl.BlockSpec((tile, 128), lambda i: (i, 0)),
                pl.BlockSpec((CHOSEN, qblocks), lambda i: (0, 0)),
                pl.BlockSpec((CHOSEN, qblocks), lambda i: (0, 0)),
            ],
            out_specs=[
                pl.BlockSpec((tile, 128), lambda i: (i, 0)),
                pl.BlockSpec((tile, 128), lambda i: (i, 0)),
                pl.BlockSpec((NZ * NX, qblocks), lambda i: (0, 0)),
            ],
        ),
        out_shape=[
            jax.ShapeDtypeStruct((tok_count, 128), jnp.bfloat16),
            jax.ShapeDtypeStruct((tok_count, 128), jnp.bfloat16),
            jax.ShapeDtypeStruct((NZ * NX, qblocks), jnp.int32),
        ],
    )(row_data, key_weight, value_weight, cosine, sine, chosen_owner[0].T, chosen_part[0].T)

    vmem = pl.BlockSpec(memory_space=pltpu.VMEM)
    smem = pl.BlockSpec(memory_space=pltpu.SMEM)
    anyspace = pl.BlockSpec(memory_space=pl.ANY)

    def chunks(count):
        return pltpu.VMEM((count, PARTS, KEY_BLOCK, 128), jnp.bfloat16)

    def picks(count):
        return pltpu.VMEM((count, ROWS, KEY_BLOCK, 128), jnp.bfloat16)

    def sems(*shape):
        return pltpu.SemaphoreType.DMA(shape)

    mixed_rows = pl.pallas_call(
        exchange_kernel,
        in_specs=[smem, vmem, vmem, vmem, vmem, anyspace, anyspace],
        out_specs=vmem,
        out_shape=jax.ShapeDtypeStruct((tok_count, WIDTH), jnp.bfloat16),
        scratch_shapes=[
            pltpu.VMEM((tok_count, D), jnp.bfloat16),
            pltpu.VMEM((D, WIDTH), jnp.bfloat16),
            pltpu.VMEM((ROWS, 2, 128, WIDTH), jnp.bfloat16),
            pltpu.VMEM((ROWS, 2, 1, WIDTH), jnp.float32),
            pltpu.VMEM((ROWS, 2, SUMS, WIDTH), jnp.float32),
            pltpu.VMEM((PARTS, KEY_BLOCK, 128), jnp.bfloat16),
            chunks(7), chunks(7), chunks(6), chunks(6),
            picks(8), picks(8), picks(6), picks(6),
            picks(8), picks(8), picks(2), picks(2), picks(2), picks(2), picks(6), picks(6),
            picks(8), picks(8), picks(2), picks(2), picks(8), picks(8), picks(2), picks(2),
            sems(2),
            sems(2, 4, 4), sems(2, 4, 4),
            sems(2), sems(2),
            sems(2, 8, 4), sems(2, 8, 4),
            sems(2, 2), sems(2, 2),
        ],
        compiler_params=pltpu.CompilerParams(collective_id=0, has_side_effects=True),
    )(table, keys.reshape(PARTS, KEY_BLOCK, 128), values.reshape(PARTS, KEY_BLOCK, 128),
      cosine, sine, row_data, query_weight)

    terms = jnp.dot(mixed_rows, out_weight, preferred_element_type=jnp.float32)
    projected = summed_on_arrival(terms.astype(jnp.bfloat16), "tp", 1)
    row_total = lax.psum(jnp.sum(projected * projected, axis=1), "tp")
    scale_rows = lax.rsqrt(row_total / D + norm_eps)
    result = (projected * scale_rows[:, None] * norm_gain[None, :]).astype(jnp.bfloat16)
    return result[None]


def solution(mesh):
    placed = (
        P("dp", "kv", None),
        P(None, "tp"),
        P(None, "tp"),
        P(None, "tp"),
        P("tp", None),
        P("tp"),
        P("dp", None, None),
        P("dp", None, None),
    )
    return jax.shard_map(
        body, mesh=mesh, in_specs=placed, out_specs=P("dp", "kv", "tp"), check_vma=False
    )
```
